32 devices in a mesh: kv: 8 (over z, y), tp: 4 (over x, core).
Axes of the slice: x: 2, y: 2, z: 4, core: 2. Of those that a mesh axis runs over, the one named last changes fastest.
Arguments:
- tokens: bfloat16 [128, 4096], P('kv'), may hold values from -6 to 6
- dec_tokens: bfloat16 [8, 4096], P('kv'), may hold values from -6 to 6
- norm_gain: float32 [4096], replicated, may hold values from 0.1 to 1.9
- w_query: bfloat16 [2, 4096, 1024], P(None, None, 'tp'), may hold values from -0.09375 to 0.09375
- w_key: bfloat16 [2, 4096, 1024], P(None, None, 'tp'), may hold values from -0.15625 to 0.15625
- w_value: bfloat16 [4096, 2048], P(None, 'tp'), may hold values from -0.09375 to 0.09375
- w_out: bfloat16 [2048, 4096], P('tp'), may hold values from -0.125 to 0.125
- head_gain: float32 [256], replicated, may hold values from 0.1 to 1.9
- mix_lambda: float32 [8], P('tp'), may hold values from 0.3 to 0.8
- ctx_keys: bfloat16 [2, 8192, 1024], P(None, 'kv', 'tp'), may hold values from -600 to 600
- ctx_values: bfloat16 [8192, 2048], P('kv', 'tp'), may hold values from -6 to 6
- dec_keys: bfloat16 [2, 8, 2048, 1024], P(None, 'kv', None, 'tp'), may hold values from -600 to 600
- dec_values: bfloat16 [8, 2048, 2048], P('kv', None, 'tp'), may hold values from -6 to 6
- dec_len: int32 [8], P('kv'), may hold values from 256 to 2048, as said below
Outputs:
- piece_out: bfloat16 [128, 4096], P('kv', 'tp')
- dec_out: bfloat16 [8, 4096], P('kv', 'tp')
The draws below stay inside these ranges and needn't reach their ends.
Inputs may be any that keep to these rules, and one draw needn't show every extreme that they name: `dec_len`: some decoding sequence has exactly 2048 cached positions.
All inputs are finite; a program needn't handle non-finite values.
Results may differ from the reference program's by a relative error of at most 0.03.
The reference program's roundings to bfloat16 on the way count: a program that leaves them out, or rounds other values in their place, can miss the bound.
Values may be sent and summed in bfloat16 or wider, within the bound.
A program may use at most 64 MiB of HBM per device.

```python
import jax
import jax.numpy as jnp
from jax import lax

D = 4096
HEADS = 8
DH = 128
DLEN = 2048
P_SIZE = 128
CTX = 8192
DECS = 8
N_TP = 4


def key_field(key, shape):
    base = jnp.clip(jax.random.normal(key, shape, jnp.float32), -6.0, 6.0) * 1.75
    return base.astype(jnp.bfloat16)


def draw_ctx_keys(key, part):
    return key_field(key, (2, CTX, HEADS * DH))


def draw_dec_keys(key, part):
    return key_field(key, (2, DECS, DLEN, HEADS * DH))


def draw_dec_len(key, part):
    lengths = jax.random.randint(key, (DECS,), DLEN // 8, DLEN + 1)
    chosen = jax.random.randint(jax.random.fold_in(key, 3), (), 0, DECS)
    return jnp.where(jnp.arange(DECS) == chosen, DLEN, lengths).astype(jnp.int32)


def block_scale(stream_key, shape, cuts, smallest, largest):
    def one(axis_at, blocks):
        heights = jax.random.uniform(jax.random.fold_in(jax.random.fold_in(stream_key, 6), axis_at), (blocks,), jnp.float32, smallest / len(cuts), largest / len(cuts))
        return jnp.repeat(jnp.exp(heights), shape[axis_at] // blocks).reshape((-1,) + (1,) * (len(shape) - axis_at - 1))

    loudness = one(*cuts[0])
    for cut in cuts[1:]:
        loudness = loudness * one(*cut)
    return loudness


def bell_draw(key, extent, scale, bound, shards=(), kind=jnp.bfloat16):
    loudness = block_scale(key, extent, shards, -0.22, 0.18) if shards else 1.0
    values = jax.random.normal(key, extent, jnp.float32) * scale * loudness
    return jnp.minimum(jnp.maximum(values, -bound), bound).astype(kind)


def setup_inputs(seed: int = 0) -> dict:
    seeds = jax.random.split(jax.random.key(seed), 15)
    return {
        "tokens": bell_draw(seeds[0], (P_SIZE, D), 1.0, 6.0, ((0, 8),)),
        "dec_tokens": bell_draw(seeds[1], (DECS, D), 1.0, 6.0, ((0, 8),)),
        "norm_gain": jnp.clip(1.0 + 0.18 * jax.random.normal(seeds[2], (D,), jnp.float32), 0.1, 1.9),
        "w_query": bell_draw(seeds[3], (2, D, HEADS * DH), D ** -0.5, 0.09375, ((2, 4),)),
        "w_key": bell_draw(seeds[4], (2, D, HEADS * DH), (D // 3) ** -0.5, 0.15625, ((2, 4),)),
        "w_value": bell_draw(seeds[5], (D, HEADS * 2 * DH), D ** -0.5, 0.09375, ((1, 4),)),
        "w_out": bell_draw(seeds[6], (HEADS * 2 * DH, D), (HEADS * 2 * DH) ** -0.5, 0.125, ((0, 4),)),
        "head_gain": jnp.clip(1.0 + 0.18 * jax.random.normal(seeds[7], (2 * DH,), jnp.float32), 0.1, 1.9),
        "mix_lambda": jnp.clip(0.3 + 0.5 * jax.random.uniform(seeds[8], (HEADS,), jnp.float32) ** block_scale(seeds[8], (HEADS,), ((0, 4),), -0.2, 0.2), 0.3, 0.8),
        "ctx_keys": draw_ctx_keys(jax.random.fold_in(seeds[14], 71), 0),
        "ctx_values": bell_draw(seeds[10], (CTX, HEADS * 2 * DH), 1.0, 6.0, ((0, 8), (1, 4))),
        "dec_keys": draw_dec_keys(jax.random.fold_in(seeds[14], 71), 0),
        "dec_values": bell_draw(seeds[12], (DECS, DLEN, HEADS * 2 * DH), 1.0, 6.0, ((0, 8), (2, 4))),
        "dec_len": draw_dec_len(jax.random.fold_in(seeds[14], 71), 0),
    }


epsilon = 1e-06

def input_rows(rows, norm_gain, w_query, w_key, w_value):
    xf = rows.astype(jnp.float32)
    normed = (xf * lax.rsqrt(lax.optimization_barrier(jnp.mean(xf * xf, axis=-1, keepdims=True)) + epsilon) * norm_gain).astype(jnp.bfloat16)
    query = jnp.stack([jnp.dot(normed, w_query[c], preferred_element_type=jnp.float32) for c in range(2)], 1).astype(jnp.bfloat16)
    keys = jnp.stack([jnp.dot(normed, w_key[c], preferred_element_type=jnp.float32) for c in range(2)], 1).astype(jnp.bfloat16)
    value = jnp.dot(normed, w_value, preferred_element_type=jnp.float32).astype(jnp.bfloat16)
    return (query, keys, value)

def reference(tokens, dec_tokens, norm_gain, w_query, w_key, w_value, w_out, head_gain, mix_lambda, ctx_keys, ctx_values, dec_keys, dec_values, dec_len):
    scale = DH ** (-0.5)
    p_query, p_keys, p_value = input_rows(tokens, norm_gain, w_query, w_key, w_value)
    d_query, d_keys, d_value = input_rows(dec_tokens, norm_gain, w_query, w_key, w_value)
    all_keys = jnp.concatenate([ctx_keys.reshape(2, CTX, HEADS, DH), p_keys.reshape(P_SIZE, 2, HEADS, DH).transpose(1, 0, 2, 3)], axis=1)
    all_keys = all_keys.transpose(2, 0, 1, 3)
    all_values = jnp.concatenate([ctx_values.reshape(CTX, HEADS, 2 * DH), p_value.reshape(P_SIZE, HEADS, 2 * DH)], axis=0)
    all_values = all_values.transpose(1, 0, 2)
    key_pos = jnp.concatenate([jnp.full((CTX,), -1, jnp.int32), jnp.arange(P_SIZE, dtype=jnp.int32)])
    heads_query = p_query.reshape(P_SIZE, 2, HEADS, DH).transpose(2, 1, 0, 3)
    block = 1
    for size in (256, 128, 64, 32, 16, 8, 4, 2, 1):
        if P_SIZE % size == 0 and block == 1:
            block = size
    blocks = P_SIZE // block

    def one_head(args):
        query_h, keys_h, values_h, lam = args
        query_b = query_h.reshape(2, blocks, block, DH).transpose(1, 0, 2, 3)
        pos_b = jnp.arange(P_SIZE, dtype=jnp.int32).reshape(blocks, block)

        def one_block(inner):
            qb, qpos = inner
            valid = key_pos[None, :] <= qpos[:, None]
            probs = []
            for c in range(2):
                scores = jnp.dot(qb[c], keys_h[c].T, preferred_element_type=jnp.float32) * scale
                scores = jnp.where(valid, scores, -jnp.inf)
                top = lax.optimization_barrier(jnp.max(scores, axis=-1, keepdims=True))
                expo = jnp.exp(scores - top)
                probs.append(expo / lax.optimization_barrier(jnp.sum(expo, axis=-1, keepdims=True)))
            weights = (probs[0] - lam * probs[1]).astype(jnp.bfloat16)
            return jnp.dot(weights, values_h, preferred_element_type=jnp.float32)
        return lax.map(one_block, (query_b, pos_b)).reshape(P_SIZE, 2 * DH)
    piece_att = lax.map(one_head, (heads_query, all_keys, all_values, mix_lambda)).transpose(1, 0, 2)

    def one_seq(args):
        query_b, dk_b, dv_b, new_k, new_v, length = args
        keys_b = jnp.concatenate([dk_b.reshape(2, DLEN, HEADS, DH), new_k.reshape(2, 1, HEADS, DH)], axis=1)
        vals_b = jnp.concatenate([dv_b.reshape(DLEN, HEADS, 2 * DH), new_v.reshape(1, HEADS, 2 * DH)], axis=0)
        slot = jnp.arange(DLEN + 1, dtype=jnp.int32)
        valid = (slot < length) | (slot == DLEN)
        probs = []
        for c in range(2):
            scores = jnp.einsum('hd,jhd->hj', query_b[c].reshape(HEADS, DH).astype(jnp.float32), keys_b[c].astype(jnp.float32)) * scale
            scores = jnp.where(valid[None, :], scores, -jnp.inf)
            top = lax.optimization_barrier(jnp.max(scores, axis=-1, keepdims=True))
            expo = jnp.exp(scores - top)
            probs.append(expo / lax.optimization_barrier(jnp.sum(expo, axis=-1, keepdims=True)))
        weights = (probs[0] - mix_lambda[:, None] * probs[1]).astype(jnp.bfloat16)
        return jnp.einsum('hj,jhe->he', weights.astype(jnp.float32), vals_b.astype(jnp.float32))
    dec_keys_seq = dec_keys.transpose(1, 0, 2, 3)
    dec_att = lax.map(one_seq, (d_query, dec_keys_seq, dec_values, d_keys, d_value, dec_len))

    def head_norm(att):
        normed = att * lax.rsqrt(lax.optimization_barrier(jnp.mean(att * att, axis=-1, keepdims=True)) + epsilon) * head_gain
        return normed.astype(jnp.bfloat16).reshape(att.shape[0], HEADS * 2 * DH)

    def project(heads_out):
        group = HEADS // N_TP * 2 * DH
        total = jnp.zeros((heads_out.shape[0], D), jnp.float32)
        for g in range(N_TP):
            part = jnp.dot(heads_out[:, g * group:(g + 1) * group], w_out[g * group:(g + 1) * group], preferred_element_type=jnp.float32)
            part = lax.optimization_barrier(part.astype(jnp.bfloat16))
            total = total + part.astype(jnp.float32)
        return total.astype(jnp.bfloat16)
    return (project(head_norm(piece_att)), project(head_norm(dec_att)))
```

```python
import functools
import math

import jax
import jax.numpy as jnp
from jax import lax
from jax.experimental import pallas as pl
from jax.experimental.pallas import tpu as pltpu
from jax.sharding import PartitionSpec as P

DH = 128
epsilon = 1e-06
MESH = pl.DeviceIdType.MESH
F32 = jnp.float32
BF16 = jnp.bfloat16
LANES = 128
C_EXP = DH ** (-0.5) * math.log2(math.e)


def dot(a, b):
    return jnp.dot(a, b, preferred_element_type=F32)


def dot_nt(a, b):
    return lax.dot_general(a, b, (((1,), (1,)), ((), ())), preferred_element_type=F32)


def kernel(
    kv, tp,
    tokens, dec_tokens, norm_gain, w_query, w_key, w_value, w_out, head_gain,
    mix_lambda, dec_len, ctx_keys, ctx_values, dec_keys, dec_values,
    piece_out, dec_out,
    tok_v, dtok_v, gain_v, hgain_v, wq_v, wk_v, wv_v, wo_v,
    ck_v, cv_v, dk_v, dv_v,
    xs, q_all, kown, vown, e_v, st_all, att_send, att_recv, p_send, p_recv, d_send, d_recv,
    sem_small, sem_q, sem_k, sem_v, sem_o, sem_c, sem_d,
    qs_sem, qr_sem, ss_sem, sr_sem, as_sem, ar_sem, ps_sem, pr_sem, ds_sem, dr_sem,
):
    me = lax.axis_index("kv")
    mt = lax.axis_index("tp")
    rows, width = tokens.shape
    drows = dec_tokens.shape[0]
    w = w_query.shape[2]
    heads = w // DH
    ctx = ctx_keys.shape[1]
    slots = dec_keys.shape[2]
    total = rows * kv
    cols = w_out.shape[1] // tp
    blocks = total // LANES
    padded = xs.shape[0]

    small = [
        pltpu.make_async_copy(tokens, tok_v, sem_small.at[0]),
        pltpu.make_async_copy(dec_tokens, dtok_v, sem_small.at[1]),
        pltpu.make_async_copy(norm_gain, gain_v, sem_small.at[2]),
        pltpu.make_async_copy(head_gain, hgain_v, sem_small.at[3]),
    ]
    for c in small:
        c.start()

    def weight_copies(src, dst, sem, parts):
        step = width // parts
        out = []
        for c in range(2):
            row = []
            for i in range(parts):
                sl = pl.ds(i * step, step)
                row.append(
                    pltpu.make_async_copy(src.at[c, sl], dst.at[c, sl], sem.at[c * parts + i])
                )
            out.append(row)
        return out

    parts = 2
    q_copies = weight_copies(w_query, wq_v, sem_q, parts)
    k_copies = weight_copies(w_key, wk_v, sem_k, parts)
    vstep = width // 4
    v_copies = [
        pltpu.make_async_copy(
            w_value.at[pl.ds(i * vstep, vstep)], wv_v.at[pl.ds(i * vstep, vstep)], sem_v.at[i]
        )
        for i in range(4)
    ]
    ck_copies = [pltpu.make_async_copy(ctx_keys.at[c], ck_v.at[c], sem_c.at[c]) for c in range(2)]
    cv_copy = pltpu.make_async_copy(ctx_values, cv_v, sem_c.at[2])
    dk_copies = [pltpu.make_async_copy(dec_keys.at[c], dk_v.at[c], sem_d.at[c]) for c in range(2)]
    dv_copy = pltpu.make_async_copy(dec_values, dv_v, sem_d.at[2])
    wo_copies = []
    for d in range(tp):
        t = lax.rem(mt + d, tp)
        start = pl.multiple_of(t * cols, LANES)
        wo_copies.append(
            pltpu.make_async_copy(w_out.at[:, pl.ds(start, cols)], wo_v.at[d], sem_o.at[d])
        )
    for row in q_copies + k_copies:
        for c in row:
            c.start()
    for c in v_copies + dk_copies + ck_copies + [cv_copy, dv_copy] + wo_copies:
        c.start()

    barrier = pltpu.get_barrier_semaphore()
    for d in range(1, kv):
        pl.semaphore_signal(
            barrier, inc=1, device_id=(lax.rem(me + d, kv), mt), device_id_type=MESH
        )
    for d in range(1, tp):
        pl.semaphore_signal(
            barrier, inc=1, device_id=(me, lax.rem(mt + d, tp)), device_id_type=MESH
        )

    kown[...] = jnp.zeros_like(kown)
    vown[...] = jnp.zeros_like(vown)
    xs[rows:, :] = jnp.zeros((padded - rows, width), BF16)
    for c in small:
        c.wait()
    gain = gain_v[...]

    def normed(x):
        xf = x.astype(F32)
        inv = lax.rsqrt(jnp.mean(xf * xf, axis=-1, keepdims=True) + epsilon)
        return (xf * inv * gain).astype(BF16)

    xs[0:rows, :] = normed(tok_v[...])
    xs[rows : rows + drows, :] = normed(dtok_v[...])

    def project(copies, weights, c):
        step = width // parts
        acc = None
        for i in range(parts):
            copies[c][i].wait()
            term = dot(xs[:, i * step : (i + 1) * step], weights[c, i * step : (i + 1) * step, :])
            acc = term if acc is None else acc + term
        return acc.astype(BF16)

    dec_q = []
    for c in range(2):
        qc = project(q_copies, wq_v, c)
        q_all[me, :, c * w : (c + 1) * w] = qc[0:rows]
        dec_q.append(qc[rows:])
    pl.semaphore_wait(barrier, kv + tp - 2)

    def to_kv(src, dst, send, recv, d):
        return pltpu.make_async_remote_copy(
            src_ref=src, dst_ref=dst, send_sem=send.at[d], recv_sem=recv.at[d],
            device_id=(lax.rem(me + d, kv), mt), device_id_type=MESH,
        )

    q_sends = [to_kv(q_all.at[me], q_all.at[me], qs_sem, qr_sem, d) for d in range(1, kv)]
    for c in q_sends:
        c.start()

    dec_k = []
    for c in range(2):
        kc = project(k_copies, wk_v, c)
        kown[c, 0:rows, :] = kc[0:rows]
        dec_k.append(kc[rows:])
    acc = None
    for i in range(4):
        v_copies[i].wait()
        term = dot(xs[:, i * vstep : (i + 1) * vstep], wv_v[i * vstep : (i + 1) * vstep, :])
        acc = term if acc is None else acc + term
    vc = acc.astype(BF16)
    vown[0:rows, :] = vc[0:rows]
    dec_v = vc[rows:]

    group = 16
    hrow = lax.broadcasted_iota(jnp.int32, (group, w), 0)
    hcol = lax.broadcasted_iota(jnp.int32, (group, w), 1) // DH
    own_head = hrow == hcol
    row1 = lax.broadcasted_iota(jnp.int32, (group, 1), 0)
    lam_col = jnp.zeros((group, 1), F32)
    for h in range(heads):
        lam_col = jnp.where(row1 == h, mix_lambda[h], lam_col)
    for c in dk_copies:
        c.wait()
    slot_id = lax.broadcasted_iota(jnp.int32, (group, slots), 1)
    dec_far = []
    dec_near = []
    for r in range(drows):
        far_p = []
        near_p = []
        for c in range(2):
            qr = jnp.broadcast_to(dec_q[c][r : r + 1].astype(F32), (group, w))
            qr = jnp.where(own_head, qr, 0.0)
            kr = dec_k[c][r : r + 1].astype(F32)
            near = jnp.sum(qr * kr, axis=-1, keepdims=True)
            far = dot_nt(qr.astype(BF16), dk_v[c, r])
            far = jnp.where(slot_id < dec_len[r], far, -jnp.inf)
            top = jnp.maximum(jnp.max(far, axis=-1, keepdims=True), near)
            ef = jnp.exp2((far - top) * C_EXP)
            en = jnp.exp2((near - top) * C_EXP)
            den = jnp.sum(ef, axis=-1, keepdims=True) + en
            far_p.append(ef / den)
            near_p.append(en / den)
        dec_far.append((far_p[0] - lam_col * far_p[1]).astype(BF16))
        dec_near.append((near_p[0] - lam_col * near_p[1]).astype(BF16).astype(F32))

    for c in ck_copies:
        c.wait()
    for d, c in enumerate(q_sends, 1):
        c.wait_recv()
    nstat = 2 * heads
    srows = st_all.shape[1]

    def score_block(b):
        slot0 = b * (LANES // rows)
        qb = q_all[pl.ds(slot0, LANES // rows)].reshape(LANES, 2 * w)
        pos = b * LANES + lax.broadcasted_iota(jnp.int32, (LANES, LANES), 0)
        key = lax.broadcasted_iota(jnp.int32, (LANES, LANES), 1)
        ok = (key < rows) & (key + me * rows <= pos)
        lane = key
        stats = jnp.zeros((LANES, LANES), F32)
        for h in range(heads):
            for c in range(2):
                q = qb[:, c * w + h * DH : c * w + (h + 1) * DH]
                hs = slice(h * DH, (h + 1) * DH)
                far = dot_nt(q, ck_v[c, :, hs])
                near = dot_nt(q, kown[c, :, hs])
                near = jnp.where(ok, near, -jnp.inf)
                top = jnp.maximum(
                    jnp.max(far, axis=-1, keepdims=True), jnp.max(near, axis=-1, keepdims=True)
                )
                ef = jnp.exp2((far - top) * C_EXP)
                en = jnp.exp2((near - top) * C_EXP)
                tot = jnp.sum(ef, axis=-1, keepdims=True) + jnp.sum(en, axis=-1, keepdims=True)
                i = 2 * h + c
                rs = pl.ds(b * LANES, LANES)
                e_v[i, rs, 0:ctx] = ef
                e_v[i, rs, ctx:] = en
                stats = jnp.where(lane == i, top, stats)
                stats = jnp.where(lane == nstat + i, tot, stats)
        st_all[me, :, pl.ds(pl.multiple_of(b * LANES, LANES), LANES)] = stats.T[0:srows]

    def each_block(f):
        if blocks == 1:
            f(0)
        else:
            pl.loop(0, blocks)(f)

    each_block(score_block)
    st_sends = [to_kv(st_all.at[me], st_all.at[me], ss_sem, sr_sem, d) for d in range(1, kv)]
    for c in st_sends:
        c.start()

    vw = 2 * DH
    hgain = hgain_v[...]
    dv_copy.wait()
    vrow = lax.broadcasted_iota(jnp.int32, (group, heads * vw), 0)
    vcol = lax.broadcasted_iota(jnp.int32, (group, heads * vw), 1) // vw

    def head_norm(att):
        out = []
        for h in range(heads):
            a = att[:, h * vw : (h + 1) * vw]
            inv = lax.rsqrt(jnp.mean(a * a, axis=-1, keepdims=True) + epsilon)
            out.append((a * inv * hgain).astype(BF16))
        return out

    def out_project(ho, d):
        acc = None
        for h in range(heads):
            term = dot(ho[h], wo_v[d, h * vw : (h + 1) * vw, :])
            acc = term if acc is None else acc + term
        return acc.astype(BF16)

    def to_tp(src, dst, send, recv, d):
        return pltpu.make_async_remote_copy(
            src_ref=src.at[d], dst_ref=dst.at[d], send_sem=send.at[d], recv_sem=recv.at[d],
            device_id=(me, lax.rem(mt + d, tp)), device_id_type=MESH,
        )

    dec_att = []
    for r in range(drows):
        att = dot(dec_far[r], dv_v[r]) + dec_near[r] * dec_v[r : r + 1].astype(F32)
        dec_att.append(jnp.sum(jnp.where(vrow == vcol, att, 0.0), axis=0, keepdims=True))
    dec_rows = jnp.concatenate(dec_att, axis=0) if drows > 1 else dec_att[0]
    dec_ho = head_norm(jnp.broadcast_to(dec_rows, (group, heads * vw)) if drows == 1 else dec_rows)
    for c in wo_copies:
        c.wait()
    d_sends = [to_tp(d_send, d_recv, ds_sem, dr_sem, d) for d in range(1, tp)]
    for d in range(1, tp):
        d_send[d] = out_project(dec_ho, d)[0:drows]
        d_sends[d - 1].start()
    dec_own = out_project(dec_ho, 0)[0:drows]

    cv_copy.wait()
    for c in st_sends:
        c.wait_recv()

    def value_block(b):
        st = st_all[:, :, pl.ds(pl.multiple_of(b * LANES, LANES), LANES)]
        mx = st[:, 0:nstat]
        top = jnp.max(mx, axis=0)
        den = jnp.sum(st[:, nstat : 2 * nstat] * jnp.exp2((mx - top[None]) * C_EXP), axis=0)
        mine = st_all[me, 0:nstat, pl.ds(pl.multiple_of(b * LANES, LANES), LANES)]
        fac = jnp.exp2((mine - top) * C_EXP) / den
        fac = jnp.concatenate([fac, jnp.zeros((LANES - nstat, LANES), F32)], axis=0).T
        rs = pl.ds(b * LANES, LANES)
        for h in range(heads):
            f1 = fac[:, 2 * h : 2 * h + 1]
            f2 = fac[:, 2 * h + 1 : 2 * h + 2] * mix_lambda[h]
            wt = (e_v[2 * h, rs] * f1 - e_v[2 * h + 1, rs] * f2).astype(BF16)
            hv = slice(h * vw, (h + 1) * vw)
            att = dot(wt[:, 0:ctx], cv_v[:, hv]) + dot(wt[:, ctx:], vown[:, hv])
            att_send[pl.ds(b * (LANES // rows), LANES // rows), :, hv] = att.astype(BF16).reshape(
                LANES // rows, rows, vw
            )

    each_block(value_block)
    a_sends = []
    for d in range(1, kv):
        a_sends.append(
            to_kv(att_send.at[lax.rem(me + d, kv)], att_recv.at[me], as_sem, ar_sem, d)
        )
        a_sends[-1].start()
    total_att = att_send[me].astype(F32)
    for d, c in enumerate(a_sends, 1):
        c.wait_recv()
        total_att = total_att + att_recv[lax.rem(me - d + kv, kv)].astype(F32)

    ho = head_norm(total_att)
    p_sends = [to_tp(p_send, p_recv, ps_sem, pr_sem, d) for d in range(1, tp)]
    for d in range(1, tp):
        p_send[d] = out_project(ho, d)
        p_sends[d - 1].start()
    own = out_project(ho, 0).astype(F32)
    dsum = dec_own.astype(F32)
    for d in range(1, tp):
        d_sends[d - 1].wait_recv()
        dsum = dsum + d_recv[d].astype(F32)
    dec_out[...] = dsum.astype(BF16)
    for d in range(1, tp):
        p_sends[d - 1].wait_recv()
        own = own + p_recv[d].astype(F32)
    piece_out[...] = own.astype(BF16)
    for c in q_sends + st_sends + a_sends + d_sends + p_sends:
        c.wait_send()


def body(
    tokens, dec_tokens, norm_gain, w_query, w_key, w_value, w_out, head_gain, mix_lambda,
    ctx_keys, ctx_values, dec_keys, dec_values, dec_len, *, kv, tp,
):
    rows, width = tokens.shape
    drows = dec_tokens.shape[0]
    w = w_query.shape[2]
    heads = w // DH
    vwid = w_value.shape[1]
    ctx = ctx_keys.shape[1]
    slots = dec_keys.shape[2]
    total = rows * kv
    cols = w_out.shape[1] // tp
    padded = rows + -(-drows // 16) * 16
    srows = -(-4 * heads // 8) * 8
    any_spec = pl.BlockSpec(memory_space=pl.ANY)
    smem = pl.BlockSpec(memory_space=pltpu.SMEM)
    vmem = pl.BlockSpec(memory_space=pltpu.VMEM)
    dma = pltpu.SemaphoreType.DMA
    V = pltpu.VMEM
    return pl.pallas_call(
        functools.partial(kernel, kv, tp),
        out_shape=(
            jax.ShapeDtypeStruct((rows, cols), BF16),
            jax.ShapeDtypeStruct((drows, cols), BF16),
        ),
        in_specs=[any_spec] * 8 + [smem] * 2 + [any_spec] * 4,
        out_specs=(vmem, vmem),
        scratch_shapes=[
            V((rows, width), BF16), V((drows, width), BF16), V((1, width), F32),
            V((1, 2 * DH), F32),
            V((2, width, w), BF16), V((2, width, w), BF16), V((width, vwid), BF16),
            V((tp, vwid, cols), BF16),
            V((2, ctx, w), BF16), V((ctx, vwid), BF16),
            V((2, drows, slots, w), BF16), V((drows, slots, vwid), BF16),
            V((padded, width), BF16), V((kv, rows, 2 * w), BF16),
            V((2, LANES, w), BF16), V((LANES, vwid), BF16),
            V((2 * heads, total, ctx + LANES), F32),
            V((kv, srows, total), F32),
            V((kv, rows, vwid), BF16), V((kv, rows, vwid), BF16),
            V((tp, rows, cols), BF16), V((tp, rows, cols), BF16),
            V((tp, drows, cols), BF16), V((tp, drows, cols), BF16),
            dma((4,)), dma((4,)), dma((4,)), dma((4,)), dma((tp,)), dma((3,)), dma((3,)),
            dma((kv,)), dma((kv,)), dma((kv,)), dma((kv,)), dma((kv,)), dma((kv,)),
            dma((tp,)), dma((tp,)), dma((tp,)), dma((tp,)),
        ],
        compiler_params=pltpu.CompilerParams(
            collective_id=0, has_side_effects=True, vmem_limit_bytes=60 * 1024 * 1024
        ),
    )(
        tokens, dec_tokens, norm_gain.reshape(1, width), w_query, w_key, w_value, w_out,
        head_gain.reshape(1, 2 * DH), mix_lambda, dec_len, ctx_keys, ctx_values, dec_keys,
        dec_values,
    )


def solution(mesh):
    in_specs = (
        P("kv", None),
        P("kv", None),
        P(),
        P(None, None, "tp"),
        P(None, None, "tp"),
        P(None, "tp"),
        P("tp", None),
        P(),
        P("tp"),
        P(None, "kv", "tp"),
        P("kv", "tp"),
        P(None, "kv", None, "tp"),
        P("kv", None, "tp"),
        P("kv"),
    )
    out_specs = (P("kv", "tp"), P("kv", "tp"))
    step = functools.partial(body, kv=mesh.shape["kv"], tp=mesh.shape["tp"])
    return jax.shard_map(step, mesh=mesh, in_specs=in_specs, out_specs=out_specs, check_vma=False)
```

```python
import functools
import math

import jax
import jax.numpy as jnp
from jax import lax
from jax.experimental import pallas as pl
from jax.experimental.pallas import tpu as pltpu
from jax.sharding import PartitionSpec as P

DH = 128
epsilon = 1e-06
MESH = pl.DeviceIdType.MESH
F32 = jnp.float32
BF16 = jnp.bfloat16
LANES = 128
C_EXP = DH ** (-0.5) * math.log2(math.e)


def dot(a, b):
    return jnp.dot(a, b, preferred_element_type=F32)


def dot_nt(a, b):
    return lax.dot_general(a, b, (((1,), (1,)), ((), ())), preferred_element_type=F32)


def kernel(
    kv, tp,
    tokens, dec_tokens, norm_gain, w_query, w_key, w_value, w_out, head_gain,
    mix_lambda, dec_len, ctx_keys, ctx_values, dec_keys, dec_values,
    out,
    lam_s, len_s, tok_v, dtok_v, gain_v, hgain_v, wq_v, wk_v, wv_v, wo_v,
    ck_v, cv_v, dk_v, dv_v,
    xs, q_all, kown, vown, st_send, st_recv, att_send, att_recv, p_send, p_recv, d_send, d_recv,
    sem_small, sem_q, sem_k, sem_v, sem_o, sem_c, sem_d,
    qs_sem, qr_sem, ss_sem, sr_sem, as_sem, ar_sem, ps_sem, pr_sem, ds_sem, dr_sem,
):
    me = lax.axis_index("kv")
    mt = lax.axis_index("tp")
    rows, width = tokens.shape
    drows = dec_tokens.shape[0]
    w = w_query.shape[2]
    heads = w // DH
    ctx = ctx_keys.shape[1]
    slots = dec_keys.shape[2]
    total = rows * kv
    cols = w_out.shape[1] // tp
    blocks = total // LANES
    padded = xs.shape[0]

    def tp_peer(d):
        chip = lax.rem(mt // 2 + d // 2, tp // 2)
        return chip * 2 + lax.rem(mt + d, 2)

    barrier = pltpu.get_barrier_semaphore()
    for d in range(1, kv):
        pl.semaphore_signal(
            barrier, inc=1, device_id=(lax.rem(me + d, kv), mt), device_id_type=MESH
        )
    for d in range(1, tp):
        pl.semaphore_signal(
            barrier, inc=1, device_id=(me, tp_peer(d)), device_id_type=MESH
        )

    small = [
        pltpu.make_async_copy(tokens, tok_v, sem_small.at[0]),
        pltpu.make_async_copy(dec_tokens, dtok_v, sem_small.at[1]),
        pltpu.make_async_copy(norm_gain, gain_v, sem_small.at[2]),
        pltpu.make_async_copy(head_gain, hgain_v, sem_small.at[3]),
        pltpu.make_async_copy(mix_lambda, lam_s, sem_small.at[4]),
        pltpu.make_async_copy(dec_len, len_s, sem_small.at[5]),
    ]
    for c in small:
        c.start()

    def weight_copies(src, dst, sem, parts):
        step = width // parts
        out = []
        for c in range(2):
            row = []
            for i in range(parts):
                sl = pl.ds(i * step, step)
                row.append(
                    pltpu.make_async_copy(src.at[c, sl], dst.at[c, sl], sem.at[c * parts + i])
                )
            out.append(row)
        return out

    parts = 2
    q_copies = weight_copies(w_query, wq_v, sem_q, parts)
    k_copies = weight_copies(w_key, wk_v, sem_k, parts)
    vstep = width // 4
    v_copies = [
        pltpu.make_async_copy(
            w_value.at[pl.ds(i * vstep, vstep)], wv_v.at[pl.ds(i * vstep, vstep)], sem_v.at[i]
        )
        for i in range(4)
    ]
    ck_copies = [pltpu.make_async_copy(ctx_keys.at[c], ck_v.at[c], sem_c.at[c]) for c in range(2)]
    cv_copy = pltpu.make_async_copy(ctx_values, cv_v, sem_c.at[2])
    dk_copies = [pltpu.make_async_copy(dec_keys.at[c], dk_v.at[c], sem_d.at[c]) for c in range(2)]
    dv_copy = pltpu.make_async_copy(dec_values, dv_v, sem_d.at[2])
    wo_copies = []
    for d in range(tp):
        start = pl.multiple_of(tp_peer(d) * cols, LANES)
        wo_copies.append(
            pltpu.make_async_copy(w_out.at[:, pl.ds(start, cols)], wo_v.at[d], sem_o.at[d])
        )
    for row in q_copies + k_copies:
        for c in row:
            c.start()
    for c in v_copies + ck_copies + [cv_copy] + dk_copies + [dv_copy] + wo_copies:
        c.start()

    kown[...] = jnp.zeros_like(kown)
    vown[...] = jnp.zeros_like(vown)
    xs[rows:, :] = jnp.zeros((padded - rows, width), BF16)
    for c in small:
        c.wait()
    gain = gain_v[...]

    def normed(x):
        xf = x.astype(F32)
        inv = lax.rsqrt(jnp.mean(xf * xf, axis=-1, keepdims=True) + epsilon)
        return (xf * inv * gain).astype(BF16)

    xs[0:rows, :] = normed(tok_v[...])
    xs[rows : rows + drows, :] = normed(dtok_v[...])

    def project(copies, weights, c):
        step = width // parts
        acc = None
        for i in range(parts):
            copies[c][i].wait()
            term = dot(xs[:, i * step : (i + 1) * step], weights[c, i * step : (i + 1) * step, :])
            acc = term if acc is None else acc + term
        return acc.astype(BF16)

    dec_q = []
    for c in range(2):
        qc = project(q_copies, wq_v, c)
        q_all[me, :, c * w : (c + 1) * w] = qc[0:rows]
        dec_q.append(qc[rows:])
    pl.semaphore_wait(barrier, kv + tp - 2)

    def to_kv(src, dst, send, recv, d):
        return pltpu.make_async_remote_copy(
            src_ref=src, dst_ref=dst, send_sem=send.at[d], recv_sem=recv.at[d],
            device_id=(lax.rem(me + d, kv), mt), device_id_type=MESH,
        )

    q_sends = [to_kv(q_all.at[me], q_all.at[me], qs_sem, qr_sem, d) for d in range(1, kv)]
    for c in q_sends:
        c.start()

    dec_k = []
    for c in range(2):
        kc = project(k_copies, wk_v, c)
        kown[c, 0:rows, :] = kc[0:rows]
        dec_k.append(kc[rows:])
    acc = None
    for i in range(4):
        v_copies[i].wait()
        term = dot(xs[:, i * vstep : (i + 1) * vstep], wv_v[i * vstep : (i + 1) * vstep, :])
        acc = term if acc is None else acc + term
    vc = acc.astype(BF16)
    vown[0:rows, :] = vc[0:rows]
    dec_v = vc[rows:]

    for c in ck_copies:
        c.wait()
    cv_copy.wait()
    for c in q_sends:
        c.wait_recv()
    vw = 2 * DH
    nstat = 2 * heads
    per = LANES // rows

    def head_block(h, b):
        slots_b = pl.ds(b * per, per)
        qb = q_all[slots_b].reshape(LANES, 2 * w)
        pos = b * LANES + lax.broadcasted_iota(jnp.int32, (LANES, LANES), 0)
        lane = lax.broadcasted_iota(jnp.int32, (LANES, LANES), 1)
        ok = (lane < rows) & (lane + me * rows <= pos)
        if h == 0:
            stats = jnp.zeros((LANES, LANES), F32)
        else:
            stats = st_send[slots_b].reshape(LANES, LANES)
        hs = slice(h * DH, (h + 1) * DH)
        hv = slice(h * vw, (h + 1) * vw)
        for c in range(2):
            q = qb[:, c * w + h * DH : c * w + (h + 1) * DH]
            far = dot_nt(q, ck_v[c, :, hs])
            near = dot_nt(q, kown[c, :, hs])
            near = jnp.where(ok, near, -jnp.inf)
            top = jnp.maximum(
                jnp.max(far, axis=-1, keepdims=True), jnp.max(near, axis=-1, keepdims=True)
            )
            ef = jnp.exp2((far - top) * C_EXP)
            en = jnp.exp2((near - top) * C_EXP)
            tot = jnp.sum(ef, axis=-1, keepdims=True) + jnp.sum(en, axis=-1, keepdims=True)
            att = dot(ef.astype(BF16), cv_v[:, hv]) + dot(en.astype(BF16), vown[:, hv])
            att_send[h, slots_b, :, c * vw : (c + 1) * vw] = att.astype(BF16).reshape(
                per, rows, vw
            )
            i = 2 * h + c
            stats = jnp.where(lane == i, top, stats)
            stats = jnp.where(lane == nstat + i, tot, stats)
        st_send[slots_b] = stats.reshape(per, rows, LANES)

    a_sends = []
    for h in range(heads):
        if blocks == 1:
            head_block(h, 0)
        else:
            pl.loop(0, blocks)(functools.partial(head_block, h))
        if h == heads - 1:
            st_sends = []
            for d in range(1, kv):
                peer = lax.rem(me + d, kv)
                st_sends.append(to_kv(st_send.at[peer], st_recv.at[me], ss_sem, sr_sem, d))
                st_sends[-1].start()
        a_sends.append([])
        for d in range(1, kv):
            peer = lax.rem(me + d, kv)
            a_sends[h].append(
                to_kv(att_send.at[h, peer], att_recv.at[h, me], as_sem.at[h], ar_sem.at[h], d)
            )
            a_sends[h][-1].start()

    hgain = hgain_v[...]
    group = 16
    hrow = lax.broadcasted_iota(jnp.int32, (group, w), 0)
    hcol = lax.broadcasted_iota(jnp.int32, (group, w), 1) // DH
    own_head = hrow == hcol
    row1 = lax.broadcasted_iota(jnp.int32, (group, 1), 0)
    lam_col = jnp.zeros((group, 1), F32)
    for h in range(heads):
        lam_col = jnp.where(row1 == h, lam_s[h], lam_col)
    for c in dk_copies:
        c.wait()
    slot_id = lax.broadcasted_iota(jnp.int32, (group, slots), 1)
    vrow = lax.broadcasted_iota(jnp.int32, (group, heads * vw), 0)
    vcol = lax.broadcasted_iota(jnp.int32, (group, heads * vw), 1) // vw
    dec_att = []
    for r in range(drows):
        far_p = []
        near_p = []
        for c in range(2):
            qr = jnp.broadcast_to(dec_q[c][r : r + 1].astype(F32), (group, w))
            qr = jnp.where(own_head, qr, 0.0)
            kr = dec_k[c][r : r + 1].astype(F32)
            near = jnp.sum(qr * kr, axis=-1, keepdims=True)
            far = dot_nt(qr.astype(BF16), dk_v[c, r])
            far = jnp.where(slot_id < len_s[r], far, -jnp.inf)
            top = jnp.maximum(jnp.max(far, axis=-1, keepdims=True), near)
            ef = jnp.exp2((far - top) * C_EXP)
            en = jnp.exp2((near - top) * C_EXP)
            den = jnp.sum(ef, axis=-1, keepdims=True) + en
            far_p.append(ef / den)
            near_p.append(en / den)
        far_w = (far_p[0] - lam_col * far_p[1]).astype(BF16)
        near_w = (near_p[0] - lam_col * near_p[1]).astype(BF16).astype(F32)
        if r == 0:
            dv_copy.wait()
        att = dot(far_w, dv_v[r]) + near_w * dec_v[r : r + 1].astype(F32)
        dec_att.append(jnp.sum(jnp.where(vrow == vcol, att, 0.0), axis=0, keepdims=True))

    def head_norm(att, h):
        inv = lax.rsqrt(jnp.mean(att * att, axis=-1, keepdims=True) + epsilon)
        return (att * inv * hgain).astype(BF16)

    def out_project(ho, d):
        acc = None
        for h in range(heads):
            term = dot(ho[h], wo_v[d, h * vw : (h + 1) * vw, :])
            acc = term if acc is None else acc + term
        return acc.astype(BF16)

    def to_tp(src, dst, send, recv, d):
        return pltpu.make_async_remote_copy(
            src_ref=src.at[d], dst_ref=dst.at[d], send_sem=send.at[d], recv_sem=recv.at[d],
            device_id=(me, tp_peer(d)), device_id_type=MESH,
        )

    dec_rows = jnp.concatenate(dec_att, axis=0) if drows > 1 else dec_att[0]
    dec_rows = dec_rows if drows > 1 else jnp.broadcast_to(dec_rows, (group, heads * vw))
    dec_ho = [head_norm(dec_rows[:, h * vw : (h + 1) * vw], h) for h in range(heads)]
    for c in wo_copies:
        c.wait()
    order = list(range(tp - 1, 0, -1))
    d_sends = {d: to_tp(d_send, d_recv, ds_sem, dr_sem, d) for d in order}
    for d in order:
        d_send[d] = out_project(dec_ho, d)[0:drows]
        d_sends[d].start()
    dec_own = out_project(dec_ho, 0)[0:drows]

    for c in st_sends:
        c.wait_recv()
    lane = lax.broadcasted_iota(jnp.int32, (rows, LANES), 1)
    sts = {0: st_send[me]}
    for d in range(1, kv):
        sts[d] = st_recv[lax.rem(me - d + kv, kv)]
    top = sts[0]
    for d in range(1, kv):
        top = jnp.maximum(top, sts[d])
    den = jnp.zeros((rows, LANES), F32)
    fac = {}
    for d in range(kv):
        fac[d] = jnp.exp2((sts[d] - top) * C_EXP)
        den = den + fac[d] * pltpu.roll(sts[d], LANES - nstat, 1)
    den = jnp.where(lane < nstat, den, 1.0)
    part = jnp.ones((rows, LANES), F32)
    for h in range(heads):
        part = jnp.where(lane == 2 * h + 1, -lam_s[h], part)
    part = part / den
    for d in range(kv):
        fac[d] = fac[d] * part
    ho = []
    for h in range(heads):
        total_att = None
        for d in range(kv):
            if d == 0:
                blk = att_send[h, me]
            else:
                a_sends[h][d - 1].wait_recv()
                blk = att_recv[h, lax.rem(me - d + kv, kv)]
            for c in range(2):
                i = 2 * h + c
                term = fac[d][:, i : i + 1] * blk[:, c * vw : (c + 1) * vw].astype(F32)
                total_att = term if total_att is None else total_att + term
        ho.append(head_norm(total_att, h))

    p_sends = {d: to_tp(p_send, p_recv, ps_sem, pr_sem, d) for d in order}
    for d in order:
        p_send[d] = out_project(ho, d)
        p_sends[d].start()
    own = out_project(ho, 0).astype(F32)
    dsum = dec_own.astype(F32)
    for d in order:
        d_sends[d].wait_recv()
        dsum = dsum + d_recv[d].astype(F32)
    out[rows:, :] = jnp.broadcast_to(dsum, (out.shape[0] - rows, cols)).astype(BF16) if (
        drows == 1
    ) else jnp.concatenate(
        [dsum, jnp.zeros((out.shape[0] - rows - drows, cols), F32)], axis=0
    ).astype(BF16)
    for d in order:
        p_sends[d].wait_recv()
        own = own + p_recv[d].astype(F32)
    out[0:rows, :] = own.astype(BF16)
    for c in q_sends + st_sends + [c for row in a_sends for c in row]:
        c.wait_send()
    for d in order:
        d_sends[d].wait_send()
        p_sends[d].wait_send()


def body(
    tokens, dec_tokens, norm_gain, w_query, w_key, w_value, w_out, head_gain, mix_lambda,
    ctx_keys, ctx_values, dec_keys, dec_values, dec_len, *, kv, tp,
):
    rows, width = tokens.shape
    drows = dec_tokens.shape[0]
    w = w_query.shape[2]
    heads = w // DH
    vwid = w_value.shape[1]
    ctx = ctx_keys.shape[1]
    slots = dec_keys.shape[2]
    cols = w_out.shape[1] // tp
    padded = rows + -(-drows // 16) * 16
    any_spec = pl.BlockSpec(memory_space=pltpu.HBM)
    vmem = pl.BlockSpec(memory_space=pltpu.VMEM)
    dma = pltpu.SemaphoreType.DMA
    V = pltpu.VMEM
    out = pl.pallas_call(
        functools.partial(kernel, kv, tp),
        out_shape=jax.ShapeDtypeStruct((padded, cols), BF16),
        in_specs=[any_spec] * 14,
        out_specs=vmem,
        scratch_shapes=[
            pltpu.SMEM((heads,), F32), pltpu.SMEM((drows,), jnp.int32),
            V((rows, width), BF16), V((drows, width), BF16), V((1, width), F32),
            V((1, 2 * DH), F32),
            V((2, width, w), BF16), V((2, width, w), BF16), V((width, vwid), BF16),
            V((tp, vwid, cols), BF16),
            V((2, ctx, w), BF16), V((ctx, vwid), BF16),
            V((2, drows, slots, w), BF16), V((drows, slots, vwid), BF16),
            V((padded, width), BF16), V((kv, rows, 2 * w), BF16),
            V((2, LANES, w), BF16), V((LANES, vwid), BF16),
            V((kv, rows, LANES), F32), V((kv, rows, LANES), F32),
            V((heads, kv, rows, 4 * DH), BF16), V((heads, kv, rows, 4 * DH), BF16),
            V((tp, rows, cols), BF16), V((tp, rows, cols), BF16),
            V((tp, drows, cols), BF16), V((tp, drows, cols), BF16),
            dma((6,)), dma((4,)), dma((4,)), dma((4,)), dma((tp,)), dma((3,)), dma((3,)),
            dma((kv,)), dma((kv,)), dma((kv,)), dma((kv,)), dma((heads, kv)), dma((heads, kv)),
            dma((tp,)), dma((tp,)), dma((tp,)), dma((tp,)),
        ],
        compiler_params=pltpu.CompilerParams(
            collective_id=0, has_side_effects=True, vmem_limit_bytes=60 * 1024 * 1024
        ),
    )(
        tokens, dec_tokens, norm_gain.reshape(1, width), w_query, w_key, w_value, w_out,
        head_gain.reshape(1, 2 * DH), mix_lambda, dec_len, ctx_keys, ctx_values, dec_keys,
        dec_values,
    )
    return out[:rows], out[rows : rows + drows]


def solution(mesh):
    in_specs = (
        P("kv", None),
        P("kv", None),
        P(),
        P(None, None, "tp"),
        P(None, None, "tp"),
        P(None, "tp"),
        P("tp", None),
        P(),
        P("tp"),
        P(None, "kv", "tp"),
        P("kv", "tp"),
        P(None, "kv", None, "tp"),
        P("kv", None, "tp"),
        P("kv"),
    )
    out_specs = (P("kv", "tp"), P("kv", "tp"))
    step = functools.partial(body, kv=mesh.shape["kv"], tp=mesh.shape["tp"])
    return jax.shard_map(step, mesh=mesh, in_specs=in_specs, out_specs=out_specs, check_vma=False)
```

```python
import functools
import math

import jax
import jax.numpy as jnp
from jax import lax
from jax.experimental import pallas as pl
from jax.experimental.pallas import tpu as pltpu
from jax.sharding import PartitionSpec as P

DH = 128
epsilon = 1e-06
MESH = pl.DeviceIdType.MESH
F32 = jnp.float32
BF16 = jnp.bfloat16
LANES = 128
C_EXP = DH ** (-0.5) * math.log2(math.e)


def dot(a, b):
    return jnp.dot(a, b, preferred_element_type=F32)


def dot_nt(a, b):
    return lax.dot_general(a, b, (((1,), (1,)), ((), ())), preferred_element_type=F32)


def kernel(
    kv, tp,
    tokens, dec_tokens, norm_gain, w_query, w_key, w_value, w_out, head_gain,
    mix_lambda, dec_len, ctx_keys, ctx_values, dec_keys, dec_values,
    out,
    lam_s, len_s, tok_v, dtok_v, gain_v, hgain_v, wq_v, wk_v, wv_v, wo_v,
    ck_v, cv_v, dk_v, dv_v,
    xs, q_all, kown, vown, st_send, st_recv, att_send, att_recv, p_send, p_recv, d_send, d_recv,
    sem_small, sem_q, sem_k, sem_v, sem_o, sem_c, sem_d,
    qs_sem, qr_sem, ss_sem, sr_sem, as_sem, ar_sem, ps_sem, pr_sem, ds_sem, dr_sem,
):
    me = lax.axis_index("kv")
    mt = lax.axis_index("tp")
    rows, width = tokens.shape
    drows = dec_tokens.shape[0]
    w = w_query.shape[2]
    heads = w // DH
    ctx = ctx_keys.shape[1]
    slots = dec_keys.shape[2]
    total = rows * kv
    cols = w_out.shape[1] // tp
    blocks = total // LANES
    padded = xs.shape[0]

    def tp_peer(d):
        chip = lax.rem(mt // 2 + d // 2, tp // 2)
        return chip * 2 + lax.rem(mt + d, 2)

    barrier = pltpu.get_barrier_semaphore()
    for d in range(1, kv):
        pl.semaphore_signal(
            barrier, inc=1, device_id=(lax.rem(me + d, kv), mt), device_id_type=MESH
        )
    for d in range(1, tp):
        pl.semaphore_signal(
            barrier, inc=1, device_id=(me, tp_peer(d)), device_id_type=MESH
        )

    small = [
        pltpu.make_async_copy(tokens, tok_v, sem_small.at[0]),
        pltpu.make_async_copy(dec_tokens, dtok_v, sem_small.at[1]),
        pltpu.make_async_copy(norm_gain, gain_v, sem_small.at[2]),
        pltpu.make_async_copy(head_gain, hgain_v, sem_small.at[3]),
        pltpu.make_async_copy(mix_lambda, lam_s, sem_small.at[4]),
        pltpu.make_async_copy(dec_len, len_s, sem_small.at[5]),
    ]
    for c in small:
        c.start()

    def weight_copies(src, dst, sem, parts):
        step = width // parts
        out = []
        for c in range(2):
            row = []
            for i in range(parts):
                sl = pl.ds(i * step, step)
                row.append(
                    pltpu.make_async_copy(src.at[c, sl], dst.at[c, sl], sem.at[c * parts + i])
                )
            out.append(row)
        return out

    parts = 2
    q_copies = weight_copies(w_query, wq_v, sem_q, parts)
    k_copies = weight_copies(w_key, wk_v, sem_k, parts)
    vstep = width // 4
    v_copies = [
        pltpu.make_async_copy(
            w_value.at[pl.ds(i * vstep, vstep)], wv_v.at[pl.ds(i * vstep, vstep)], sem_v.at[i]
        )
        for i in range(4)
    ]
    ck_copies = [pltpu.make_async_copy(ctx_keys.at[c], ck_v.at[c], sem_c.at[c]) for c in range(2)]
    cv_copy = pltpu.make_async_copy(ctx_values, cv_v, sem_c.at[2])
    dk_copies = [pltpu.make_async_copy(dec_keys.at[c], dk_v.at[c], sem_d.at[c]) for c in range(2)]
    dv_copy = pltpu.make_async_copy(dec_values, dv_v, sem_d.at[2])
    wo_copies = []
    for d in range(tp):
        start = pl.multiple_of(tp_peer(d) * cols, LANES)
        wo_copies.append(
            pltpu.make_async_copy(w_out.at[:, pl.ds(start, cols)], wo_v.at[d], sem_o.at[d])
        )
    k_flat = [c for row in k_copies for c in row]
    stages = [
        [c for row in q_copies for c in row],
        k_flat,
        v_copies,
        ck_copies + [cv_copy],
        dk_copies + [dv_copy],
        wo_copies,
    ]

    def start_stage(i):
        for c in stages[i]:
            c.start()

    start_stage(0)

    kown[...] = jnp.zeros_like(kown)
    vown[...] = jnp.zeros_like(vown)
    xs[rows:, :] = jnp.zeros((padded - rows, width), BF16)
    for c in small:
        c.wait()
    gain = gain_v[...]

    def normed(x):
        xf = x.astype(F32)
        inv = lax.rsqrt(jnp.mean(xf * xf, axis=-1, keepdims=True) + epsilon)
        return (xf * inv * gain).astype(BF16)

    xs[0:rows, :] = normed(tok_v[...])
    xs[rows : rows + drows, :] = normed(dtok_v[...])

    def project(copies, weights, c):
        step = width // parts
        acc = None
        for i in range(parts):
            copies[c][i].wait()
            term = dot(xs[:, i * step : (i + 1) * step], weights[c, i * step : (i + 1) * step, :])
            acc = term if acc is None else acc + term
        return acc.astype(BF16)

    dec_q = []
    for c in range(2):
        qc = project(q_copies, wq_v, c)
        q_all[me, :, c * w : (c + 1) * w] = qc[0:rows]
        dec_q.append(qc[rows:])
        start_stage(1 + c)
        if c == 1:
            start_stage(3)
    pl.semaphore_wait(barrier, kv + tp - 2)

    def to_kv(src, dst, send, recv, d):
        return pltpu.make_async_remote_copy(
            src_ref=src, dst_ref=dst, send_sem=send.at[d], recv_sem=recv.at[d],
            device_id=(lax.rem(me + d, kv), mt), device_id_type=MESH,
        )

    far_first = sorted(range(1, kv), key=lambda d: (-min(d, kv - d), d))
    q_sends = [to_kv(q_all.at[me], q_all.at[me], qs_sem, qr_sem, d) for d in far_first]
    for c in q_sends:
        c.start()

    dec_k = []
    for c in range(2):
        kc = project(k_copies, wk_v, c)
        kown[c, 0:rows, :] = kc[0:rows]
        dec_k.append(kc[rows:])
        start_stage(4 + c)
    acc = None
    for i in range(4):
        v_copies[i].wait()
        term = dot(xs[:, i * vstep : (i + 1) * vstep], wv_v[i * vstep : (i + 1) * vstep, :])
        acc = term if acc is None else acc + term
    vc = acc.astype(BF16)
    vown[0:rows, :] = vc[0:rows]
    dec_v = vc[rows:]

    for c in ck_copies:
        c.wait()
    cv_copy.wait()
    for c in q_sends:
        c.wait_recv()
    vw = 2 * DH
    nstat = 2 * heads
    per = LANES // rows

    def head_block(h, b):
        slots_b = pl.ds(b * per, per)
        qb = q_all[slots_b].reshape(LANES, 2 * w)
        pos = b * LANES + lax.broadcasted_iota(jnp.int32, (LANES, LANES), 0)
        lane = lax.broadcasted_iota(jnp.int32, (LANES, LANES), 1)
        ok = (lane < rows) & (lane + me * rows <= pos)
        if h == 0:
            stats = jnp.zeros((LANES, LANES), F32)
        else:
            stats = st_send[slots_b].reshape(LANES, LANES)
        hs = slice(h * DH, (h + 1) * DH)
        hv = slice(h * vw, (h + 1) * vw)
        for c in range(2):
            q = qb[:, c * w + h * DH : c * w + (h + 1) * DH]
            far = dot_nt(q, ck_v[c, :, hs])
            near = dot_nt(q, kown[c, :, hs])
            near = jnp.where(ok, near, -jnp.inf)
            top = jnp.maximum(
                jnp.max(far, axis=-1, keepdims=True), jnp.max(near, axis=-1, keepdims=True)
            )
            ef = jnp.exp2((far - top) * C_EXP)
            en = jnp.exp2((near - top) * C_EXP)
            tot = jnp.sum(ef, axis=-1, keepdims=True) + jnp.sum(en, axis=-1, keepdims=True)
            att = dot(ef.astype(BF16), cv_v[:, hv]) + dot(en.astype(BF16), vown[:, hv])
            att_send[h, slots_b, :, c * vw : (c + 1) * vw] = att.astype(BF16).reshape(
                per, rows, vw
            )
            i = 2 * h + c
            stats = jnp.where(lane == i, top, stats)
            stats = jnp.where(lane == nstat + i, tot, stats)
        st_send[slots_b] = stats.reshape(per, rows, LANES)

    a_sends = []
    for h in range(heads):
        if blocks == 1:
            head_block(h, 0)
        else:
            pl.loop(0, blocks)(functools.partial(head_block, h))
        if h == heads - 1:
            st_sends = []
            for d in far_first:
                peer = lax.rem(me + d, kv)
                st_sends.append(to_kv(st_send.at[peer], st_recv.at[me], ss_sem, sr_sem, d))
                st_sends[-1].start()
        a_sends.append({})
        for d in far_first:
            peer = lax.rem(me + d, kv)
            a_sends[h][d] = to_kv(
                att_send.at[h, peer], att_recv.at[h, me], as_sem.at[h], ar_sem.at[h], d
            )
            a_sends[h][d].start()

    hgain = hgain_v[...]
    group = 16
    hrow = lax.broadcasted_iota(jnp.int32, (group, w), 0)
    hcol = lax.broadcasted_iota(jnp.int32, (group, w), 1) // DH
    own_head = hrow == hcol
    row1 = lax.broadcasted_iota(jnp.int32, (group, 1), 0)
    lam_col = jnp.zeros((group, 1), F32)
    for h in range(heads):
        lam_col = jnp.where(row1 == h, lam_s[h], lam_col)
    for c in dk_copies:
        c.wait()
    slot_id = lax.broadcasted_iota(jnp.int32, (group, slots), 1)
    vrow = lax.broadcasted_iota(jnp.int32, (group, heads * vw), 0)
    vcol = lax.broadcasted_iota(jnp.int32, (group, heads * vw), 1) // vw
    dec_att = []
    for r in range(drows):
        far_p = []
        near_p = []
        for c in range(2):
            qr = jnp.broadcast_to(dec_q[c][r : r + 1].astype(F32), (group, w))
            qr = jnp.where(own_head, qr, 0.0)
            kr = dec_k[c][r : r + 1].astype(F32)
            near = jnp.sum(qr * kr, axis=-1, keepdims=True)
            far = dot_nt(qr.astype(BF16), dk_v[c, r])
            far = jnp.where(slot_id < len_s[r], far, -jnp.inf)
            top = jnp.maximum(jnp.max(far, axis=-1, keepdims=True), near)
            ef = jnp.exp2((far - top) * C_EXP)
            en = jnp.exp2((near - top) * C_EXP)
            den = jnp.sum(ef, axis=-1, keepdims=True) + en
            far_p.append(ef / den)
            near_p.append(en / den)
        far_w = (far_p[0] - lam_col * far_p[1]).astype(BF16)
        near_w = (near_p[0] - lam_col * near_p[1]).astype(BF16).astype(F32)
        if r == 0:
            dv_copy.wait()
        att = dot(far_w, dv_v[r]) + near_w * dec_v[r : r + 1].astype(F32)
        dec_att.append(jnp.sum(jnp.where(vrow == vcol, att, 0.0), axis=0, keepdims=True))

    def head_norm(att, h):
        inv = lax.rsqrt(jnp.mean(att * att, axis=-1, keepdims=True) + epsilon)
        return (att * inv * hgain).astype(BF16)

    def out_project(ho, d):
        acc = None
        for h in range(heads):
            term = dot(ho[h], wo_v[d, h * vw : (h + 1) * vw, :])
            acc = term if acc is None else acc + term
        return acc.astype(BF16)

    def to_tp(src, dst, send, recv, d):
        return pltpu.make_async_remote_copy(
            src_ref=src.at[d], dst_ref=dst.at[d], send_sem=send.at[d], recv_sem=recv.at[d],
            device_id=(me, tp_peer(d)), device_id_type=MESH,
        )

    dec_rows = jnp.concatenate(dec_att, axis=0) if drows > 1 else dec_att[0]
    dec_rows = dec_rows if drows > 1 else jnp.broadcast_to(dec_rows, (group, heads * vw))
    dec_ho = [head_norm(dec_rows[:, h * vw : (h + 1) * vw], h) for h in range(heads)]
    for c in wo_copies:
        c.wait()
    order = list(range(tp - 1, 0, -1))
    d_sends = {d: to_tp(d_send, d_recv, ds_sem, dr_sem, d) for d in order}
    for d in order:
        d_send[d] = out_project(dec_ho, d)[0:drows]
        d_sends[d].start()
    dec_own = out_project(dec_ho, 0)[0:drows]

    for c in st_sends:
        c.wait_recv()
    lane = lax.broadcasted_iota(jnp.int32, (rows, LANES), 1)
    sts = {0: st_send[me]}
    for d in range(1, kv):
        sts[d] = st_recv[lax.rem(me - d + kv, kv)]
    top = sts[0]
    for d in range(1, kv):
        top = jnp.maximum(top, sts[d])
    den = jnp.zeros((rows, LANES), F32)
    fac = {}
    for d in range(kv):
        fac[d] = jnp.exp2((sts[d] - top) * C_EXP)
        den = den + fac[d] * pltpu.roll(sts[d], LANES - nstat, 1)
    den = jnp.where(lane < nstat, den, 1.0)
    part = jnp.ones((rows, LANES), F32)
    for h in range(heads):
        part = jnp.where(lane == 2 * h + 1, -lam_s[h], part)
    part = part / den
    for d in range(kv):
        fac[d] = fac[d] * part
    ho = []
    for h in range(heads):
        total_att = None
        for d in range(kv):
            if d == 0:
                blk = att_send[h, me]
            else:
                a_sends[h][d].wait_recv()
                blk = att_recv[h, lax.rem(me - d + kv, kv)]
            for c in range(2):
                i = 2 * h + c
                term = fac[d][:, i : i + 1] * blk[:, c * vw : (c + 1) * vw].astype(F32)
                total_att = term if total_att is None else total_att + term
        ho.append(head_norm(total_att, h))

    p_sends = {d: to_tp(p_send, p_recv, ps_sem, pr_sem, d) for d in order}
    for d in order:
        p_send[d] = out_project(ho, d)
        p_sends[d].start()
    own = out_project(ho, 0).astype(F32)
    dsum = dec_own.astype(F32)
    for d in order:
        d_sends[d].wait_recv()
        dsum = dsum + d_recv[d].astype(F32)
    out[rows:, :] = jnp.broadcast_to(dsum, (out.shape[0] - rows, cols)).astype(BF16) if (
        drows == 1
    ) else jnp.concatenate(
        [dsum, jnp.zeros((out.shape[0] - rows - drows, cols), F32)], axis=0
    ).astype(BF16)
    for d in order:
        p_sends[d].wait_recv()
        own = own + p_recv[d].astype(F32)
    out[0:rows, :] = own.astype(BF16)
    for c in q_sends + st_sends + [c for row in a_sends for c in row.values()]:
        c.wait_send()
    for d in order:
        d_sends[d].wait_send()
        p_sends[d].wait_send()


def body(
    tokens, dec_tokens, norm_gain, w_query, w_key, w_value, w_out, head_gain, mix_lambda,
    ctx_keys, ctx_values, dec_keys, dec_values, dec_len, *, kv, tp,
):
    rows, width = tokens.shape
    drows = dec_tokens.shape[0]
    w = w_query.shape[2]
    heads = w // DH
    vwid = w_value.shape[1]
    ctx = ctx_keys.shape[1]
    slots = dec_keys.shape[2]
    cols = w_out.shape[1] // tp
    padded = rows + -(-drows // 16) * 16
    any_spec = pl.BlockSpec(memory_space=pltpu.HBM)
    vmem = pl.BlockSpec(memory_space=pltpu.VMEM)
    dma = pltpu.SemaphoreType.DMA
    V = pltpu.VMEM
    out = pl.pallas_call(
        functools.partial(kernel, kv, tp),
        out_shape=jax.ShapeDtypeStruct((padded, cols), BF16),
        in_specs=[any_spec] * 14,
        out_specs=vmem,
        scratch_shapes=[
            pltpu.SMEM((heads,), F32), pltpu.SMEM((drows,), jnp.int32),
            V((rows, width), BF16), V((drows, width), BF16), V((1, width), F32),
            V((1, 2 * DH), F32),
            V((2, width, w), BF16), V((2, width, w), BF16), V((width, vwid), BF16),
            V((tp, vwid, cols), BF16),
            V((2, ctx, w), BF16), V((ctx, vwid), BF16),
            V((2, drows, slots, w), BF16), V((drows, slots, vwid), BF16),
            V((padded, width), BF16), V((kv, rows, 2 * w), BF16),
            V((2, LANES, w), BF16), V((LANES, vwid), BF16),
            V((kv, rows, LANES), F32), V((kv, rows, LANES), F32),
            V((heads, kv, rows, 4 * DH), BF16), V((heads, kv, rows, 4 * DH), BF16),
            V((tp, rows, cols), BF16), V((tp, rows, cols), BF16),
            V((tp, drows, cols), BF16), V((tp, drows, cols), BF16),
            dma((6,)), dma((4,)), dma((4,)), dma((4,)), dma((tp,)), dma((3,)), dma((3,)),
            dma((kv,)), dma((kv,)), dma((kv,)), dma((kv,)), dma((heads, kv)), dma((heads, kv)),
            dma((tp,)), dma((tp,)), dma((tp,)), dma((tp,)),
        ],
        compiler_params=pltpu.CompilerParams(
            collective_id=0, has_side_effects=True, vmem_limit_bytes=60 * 1024 * 1024
        ),
    )(
        tokens, dec_tokens, norm_gain.reshape(1, width), w_query, w_key, w_value, w_out,
        head_gain.reshape(1, 2 * DH), mix_lambda, dec_len, ctx_keys, ctx_values, dec_keys,
        dec_values,
    )
    def split(src, piece_ref, dec_ref):
        piece_ref[...] = src[0:rows, :]
        dec_ref[...] = src[rows : rows + drows, :]

    return pl.pallas_call(
        split,
        out_shape=(
            jax.ShapeDtypeStruct((rows, cols), BF16),
            jax.ShapeDtypeStruct((drows, cols), BF16),
        ),
        in_specs=[vmem],
        out_specs=(vmem, vmem),
    )(out)


def solution(mesh):
    in_specs = (
        P("kv", None),
        P("kv", None),
        P(),
        P(None, None, "tp"),
        P(None, None, "tp"),
        P(None, "tp"),
        P("tp", None),
        P(),
        P("tp"),
        P(None, "kv", "tp"),
        P("kv", "tp"),
        P(None, "kv", None, "tp"),
        P("kv", None, "tp"),
        P("kv"),
    )
    out_specs = (P("kv", "tp"), P("kv", "tp"))
    step = functools.partial(body, kv=mesh.shape["kv"], tp=mesh.shape["tp"])
    return jax.shard_map(step, mesh=mesh, in_specs=in_specs, out_specs=out_specs, check_vma=False)
```
